32 devices in a mesh: grp: 2 (over y), ra: 4 (over z), cb: 4 (over x, core).
Axes of the slice: x: 2, y: 2, z: 4, core: 2. Of those that a mesh axis runs over, the one named last changes fastest.
Arguments:
- tokens: bfloat16 [1024, 4096], P('grp', 'ra'), parts along dimension 0, may hold values from -14 to 14
- pre_gain: bfloat16 [2, 4096], P(None, 'ra'), may hold values from 0.099609375 to 1.8984375
- post_gain: bfloat16 [2, 4096], P(None, 'ra'), may hold values from 0.099609375 to 1.8984375
- gate_weight: bfloat16 [2, 4096, 11008], P(None, 'ra', 'cb'), may hold values from -0.09375 to 0.09375
- up_weight: bfloat16 [2, 4096, 11008], P(None, 'ra', 'cb'), may hold values from -0.09375 to 0.09375
- gate_taps: bfloat16 [2, 3, 11008], P(None, None, 'cb'), may hold values from -3 to 3
- up_taps: bfloat16 [2, 3, 11008], P(None, None, 'cb'), may hold values from -3 to 3
- gate_bias: bfloat16 [2, 11008], P(None, 'cb'), may hold values from -3 to 3
- up_bias: bfloat16 [2, 11008], P(None, 'cb'), may hold values from -3 to 3
- down_weight: bfloat16 [2, 11008, 4096], P(None, 'cb', 'ra'), may hold values from -0.07624929 to 0.07624929
Outputs:
- layer_out: bfloat16 [1024, 4096], P('grp', 'ra'), parts along dimension 0
The draws below stay inside these ranges and needn't reach their ends.
There are 2 independent parts, one for each index of `grp`. The reference program is written for one: setup_inputs(seed, part) draws one part's arguments, and reference() takes and returns one part's arrays. A program takes and returns all parts, laid end to end along the dimension named above; an argument that names none is the same for every part. Nothing has to cross between parts.
All inputs are finite; a program needn't handle non-finite values.
Results may differ from the reference program's by a relative error of at most 0.024.
Values may be sent and summed in bfloat16 or wider, within the bound.
A program may use at most 128 MiB of HBM per device.

```python
import jax
import jax.numpy as jnp
from jax import lax

D = 4096
FF = 11008
TAPS = 3
LAYERS = 2
SEQS = 2
TOKENS = 512
HID_BLOCK = 2752
N_CB = 4


def draw_tokens(key, part):
    key_rows, key_cols, key_vals = jax.random.split(jax.random.fold_in(key, 11), 3)
    position = jnp.arange(D, dtype=jnp.float32)[None, :] / D
    row_log = jax.random.uniform(key_rows, (TOKENS, 1), jnp.float32, -0.5, 0.5) * jnp.log(10.0)
    col_log = (0.5 * position + 0.5 * jax.random.uniform(key_cols, (1, D), jnp.float32) - 0.5) * jnp.log(10.0)
    entries = jnp.clip(jax.random.normal(key_vals, (TOKENS, D), jnp.float32), -4.0, 4.0)
    return (entries * jnp.exp(row_log) * jnp.exp(col_log) / 3.0).astype(jnp.bfloat16)


def draw_down_weight(key, part):
    key_cols, key_vals = jax.random.split(jax.random.fold_in(key, 23), 2)
    position = jnp.arange(D, dtype=jnp.float32)[None, None, :] / D
    spread = jax.random.uniform(key_cols, (LAYERS, 1, D), jnp.float32)
    col_log = (0.5 * position + 0.5 * spread - 0.5) * jnp.log(10.0)
    entries = jnp.clip(jax.random.normal(key_vals, (LAYERS, FF, D), jnp.float32), -2.5, 2.5)
    return (entries * jnp.exp(col_log) / jnp.sqrt(jnp.float32(FF))).astype(jnp.bfloat16)


def level_of(rng, extent, cuts, least, top_value):
    level, own = 1.0, jax.random.fold_in(rng, 6)
    for axis_at, parts in cuts:
        steps = jnp.exp(jax.random.uniform(jax.random.fold_in(own, axis_at), (parts,), jnp.float32, least / len(cuts), top_value / len(cuts)))
        level = level * jnp.repeat(steps, extent[axis_at] // parts).reshape([-1 if axis == axis_at else 1 for axis in range(len(extent))])
    return level


def bell_draw(stream_key, extent, scale, bound, shards=(), kind=jnp.bfloat16):
    values = jax.random.normal(stream_key, extent, jnp.float32) * scale
    if len(shards) > 0:
        values = level_of(stream_key, extent, shards, -0.22, 0.18) * values
    return jnp.clip(values, min=-bound, max=bound).astype(kind)


def setup_inputs(seed: int = 0, part: int = 0) -> dict:
    key_of = jax.random.split(jax.random.key(seed), 11)
    part_splits = jax.random.split(jax.random.fold_in(key_of[10], part), 11)
    tokens = draw_tokens(jax.random.fold_in(jax.random.fold_in(key_of[10], part), 71), part)
    pre_gain = jnp.clip(1.0 + 0.18 * jax.random.normal(key_of[1], (LAYERS, D), jnp.float32), 0.099609375, 1.8984375).astype(jnp.bfloat16)
    post_gain = jnp.clip(1.0 + 0.18 * jax.random.normal(key_of[2], (LAYERS, D), jnp.float32), 0.099609375, 1.8984375).astype(jnp.bfloat16)
    gate_weight = bell_draw(key_of[3], (LAYERS, D, FF), D ** -0.5, 0.09375, ((1, 4), (2, 4)))
    up_weight = bell_draw(key_of[4], (LAYERS, D, FF), D ** -0.5, 0.09375, ((1, 4), (2, 4)))
    gate_taps = bell_draw(key_of[5], (LAYERS, TAPS, FF), 0.577, 3.0, ((2, 4),))
    up_taps = bell_draw(key_of[6], (LAYERS, TAPS, FF), 0.577, 3.0, ((2, 4),))
    gate_bias = bell_draw(key_of[7], (LAYERS, FF), 0.5, 3.0, ((1, 4),))
    up_bias = bell_draw(key_of[8], (LAYERS, FF), 0.5, 3.0, ((1, 4),))
    down_weight = draw_down_weight(jax.random.fold_in(key_of[10], 71), part)
    return dict(tokens=tokens, pre_gain=pre_gain, post_gain=post_gain, gate_weight=gate_weight, up_weight=up_weight, gate_taps=gate_taps, up_taps=up_taps, gate_bias=gate_bias, up_bias=up_bias, down_weight=down_weight)


epsilon = 1e-06
residual_scale = 0.5

def shift_rows(values, delay_by, sequences):
    total_rows, columns = values.shape
    per_sequence = total_rows // sequences
    grouped = values.reshape(sequences, per_sequence, columns)
    moved = jnp.pad(grouped, ((0, 0), (delay_by, 0), (0, 0)))[:, :per_sequence]
    return moved.reshape(total_rows, columns)

def causal_conv(values, tap_weights, sequences):
    tap_count = tap_weights.shape[0]
    result = tap_weights[tap_count - 1] * values
    for offset in range(1, tap_count):
        result = result + tap_weights[tap_count - 1 - offset] * shift_rows(values, offset, sequences)
    return result

def reference(tokens, pre_gain, post_gain, gate_weight, up_weight, gate_taps, up_taps, gate_bias, up_bias, down_weight):
    state = tokens
    for which_layer in range(LAYERS):
        widened = state.astype(jnp.float32)
        pre_scale = lax.rsqrt(lax.optimization_barrier(jnp.sum(widened * widened, axis=1, keepdims=True)) / D + epsilon)
        normed = (widened * pre_gain[which_layer].astype(jnp.float32)).astype(jnp.bfloat16)
        gate_lin = jnp.dot(normed, gate_weight[which_layer], preferred_element_type=jnp.float32) * pre_scale
        up_lin = jnp.dot(normed, up_weight[which_layer], preferred_element_type=jnp.float32) * pre_scale
        gate_conv = causal_conv(gate_lin, gate_taps[which_layer].astype(jnp.float32), SEQS) + gate_bias[which_layer].astype(jnp.float32)
        up_conv = causal_conv(up_lin, up_taps[which_layer].astype(jnp.float32), SEQS) + up_bias[which_layer].astype(jnp.float32)
        hidden = (jax.nn.gelu(gate_conv, approximate=True) * up_conv).astype(jnp.bfloat16)
        blocks = hidden.reshape(TOKENS, N_CB, HID_BLOCK).astype(jnp.float32)
        weights = down_weight[which_layer].reshape(N_CB, HID_BLOCK, D).astype(jnp.float32)
        partials = jnp.einsum('tkf,kfd->ktd', blocks, weights).astype(jnp.bfloat16)
        branch = lax.optimization_barrier(jnp.sum(partials.astype(jnp.float32), axis=0))
        post_scale = lax.rsqrt(lax.optimization_barrier(jnp.sum(branch * branch, axis=1, keepdims=True)) / D + epsilon)
        state = (residual_scale * widened + branch * post_scale * post_gain[which_layer].astype(jnp.float32)).astype(jnp.bfloat16)
    return state
```

```python
import functools

import jax
import jax.numpy as jnp
from jax import lax
from jax.experimental import pallas as pl
from jax.experimental.pallas import tpu as pltpu
from jax.sharding import PartitionSpec as P

LEN = 256
LANES = 128
SKEW = 2

epsilon = 1e-06
residual_scale = 0.5
MESH = pl.DeviceIdType.MESH


def hidden_kernel(
    layer, n, nch, nfull, fl,
    x_ref, scale_ref, coef_ref, tg_ref, tu_ref, wg_hbm, wu_hbm, wd_hbm,
    out_ref,
    w, wd, part, hid, acc, wsem, wdsem, part_send, part_recv, hid_send, hid_recv,
):
    z = lax.axis_index("ra")
    half = x_ref.shape[0] // 2

    def w_copies(j):
        cols = pl.ds(pl.multiple_of(j * LANES, LANES), LANES)
        return (
            pltpu.make_async_copy(
                wg_hbm.at[layer, :, cols], w.at[j, :, pl.ds(0, LANES)], wsem.at[0, j]),
            pltpu.make_async_copy(
                wu_hbm.at[layer, :, cols], w.at[j, :, pl.ds(LANES, LANES)], wsem.at[1, j]),
        )

    @pl.loop(0, nfull)
    def _(j):
        for copy in w_copies(j):
            copy.start()

    wd_copy = pltpu.make_async_copy(wd_hbm.at[layer], wd.at[pl.ds(0, fl)], wdsem)
    wd_copy.start()

    barrier = pltpu.get_barrier_semaphore()

    @pl.when(z > 0)
    def _():
        pl.semaphore_signal(barrier, inc=1, device_id={"ra": z - 1}, device_id_type=MESH)

    @pl.when(z < n - 1)
    def _():
        pl.semaphore_signal(barrier, inc=1, device_id={"ra": z + 1}, device_id_type=MESH)

    if nch > nfull:
        w[nfull, :, 0:LANES] = tg_ref[...]
        w[nfull, :, LANES:] = tu_ref[...]
        wd[fl:, :] = jnp.zeros((nch * LANES - fl, wd.shape[1]), wd.dtype)
    acc[...] = jnp.zeros_like(acc)

    inner = (z > 0) & (z < n - 1)

    @pl.when(inner)
    def _():
        pl.semaphore_wait(barrier, 2)

    @pl.when(jnp.logical_not(inner))
    def _():
        pl.semaphore_wait(barrier, 1)

    def place(d):
        if d == 0:
            return n - 1 - z, z - 1, z + 1
        return z, z + 1, z - 1

    def part_copy(d, j, target):
        return pltpu.make_async_remote_copy(
            src_ref=part.at[d, j], dst_ref=part.at[d, j],
            send_sem=part_send.at[d, j], recv_sem=part_recv.at[d, j],
            device_id={"ra": target}, device_id_type=MESH)

    def hid_copy(d, j, target):
        return pltpu.make_async_remote_copy(
            src_ref=hid.at[d, j], dst_ref=hid.at[d, j],
            send_sem=hid_send.at[d, j], recv_sem=hid_recv.at[d, j],
            device_id={"ra": target}, device_id_type=MESH)

    def conv(values, taps, bias):
        rows = lax.broadcasted_iota(jnp.int32, values.shape, 0) % LEN
        count = len(taps)
        result = taps[count - 1] * values
        for offset in range(1, count):
            moved = jnp.where(rows >= offset, pltpu.roll(values, offset, 0), 0.0)
            result = result + taps[count - 1 - offset] * moved
        return result + bias

    def add_down(d, j):
        rows = slice(d * half, (d + 1) * half)
        wrows = pl.ds(pl.multiple_of(j * LANES, LANES), LANES)
        acc[rows, :] += jnp.dot(hid[d, j], wd[wrows, :], preferred_element_type=jnp.float32)

    @pl.loop(0, nch + 2 * (n - 1) * SKEW)
    def _(s):
        @pl.when(s < nfull)
        def _():
            for copy in w_copies(s):
                copy.wait()

        @pl.when(s == 1)
        def _():
            wd_copy.wait()

        for d in range(2):
            p, nxt, prv = place(d)
            rows = slice(d * half, (d + 1) * half)
            c = s - p * SKEW

            @pl.when((c >= 0) & (c < nch))
            def _():
                own = jnp.dot(x_ref[rows, :], w[c], preferred_element_type=jnp.float32)

                @pl.when(p == 0)
                def _():
                    part[d, c] = own.astype(part.dtype)
                    part_copy(d, c, nxt).start()

                @pl.when((p > 0) & (p < n - 1))
                def _():
                    part_copy(d, c, nxt).wait_recv()
                    part[d, c] = (part[d, c].astype(jnp.float32) + own).astype(part.dtype)
                    part_copy(d, c, nxt).start()

                @pl.when(p == n - 1)
                def _():
                    part_copy(d, c, prv).wait_recv()
                    total = (part[d, c].astype(jnp.float32) + own) * scale_ref[rows, :]
                    coef = coef_ref[:, pl.ds(pl.multiple_of(c * LANES, LANES), LANES)]
                    k = coef.shape[0] // 2
                    row = [coef[i : i + 1, :] for i in range(2 * k)]
                    gate = conv(total[:, :LANES], row[: k - 1], row[k - 1])
                    up = conv(total[:, LANES:], row[k : 2 * k - 1], row[2 * k - 1])
                    hid[d, c] = (jax.nn.gelu(gate, approximate=True) * up).astype(hid.dtype)
                    hid_copy(d, c, prv).start()
                    add_down(d, c)

            e = s - (2 * (n - 1) - p) * SKEW

            @pl.when((p < n - 1) & (e >= 0) & (e < nch))
            def _():
                hid_copy(d, e, nxt).wait_recv()

                @pl.when(p > 0)
                def _():
                    hid_copy(d, e, prv).start()

                add_down(d, e)

    out_ref[...] = acc[...].astype(out_ref.dtype)

    for d in range(2):
        p, nxt, prv = place(d)

        @pl.loop(0, nch)
        def _(j):
            @pl.when(p < n - 1)
            def _():
                part_copy(d, j, nxt).wait_send()

            @pl.when(p > 0)
            def _():
                hid_copy(d, j, prv).wait_send()


def down_partial(layer, n, normed, scale, coef, tg, tu, gate_weight, up_weight, down_weight):
    tokens, dl = normed.shape
    fl = gate_weight.shape[2]
    nfull = fl // LANES
    nch = -(-fl // LANES)
    half = tokens // 2
    vmem = pl.BlockSpec(memory_space=pltpu.VMEM)
    hbm = pl.BlockSpec(memory_space=pl.ANY)
    dma = pltpu.SemaphoreType.DMA
    return pl.pallas_call(
        functools.partial(hidden_kernel, layer, n, nch, nfull, fl),
        out_shape=jax.ShapeDtypeStruct((tokens, down_weight.shape[2]), jnp.bfloat16),
        in_specs=[vmem] * 5 + [hbm] * 3,
        out_specs=vmem,
        scratch_shapes=[
            pltpu.VMEM((nch, dl, 2 * LANES), jnp.bfloat16),
            pltpu.VMEM((nch * LANES, down_weight.shape[2]), jnp.bfloat16),
            pltpu.VMEM((2, nch, half, 2 * LANES), jnp.bfloat16),
            pltpu.VMEM((2, nch, half, LANES), jnp.bfloat16),
            pltpu.VMEM((tokens, down_weight.shape[2]), jnp.float32),
            dma((2, nch)),
            dma,
            dma((2, nch)),
            dma((2, nch)),
            dma((2, nch)),
            dma((2, nch)),
        ],
        compiler_params=pltpu.CompilerParams(
            collective_id=layer, has_side_effects=True, vmem_limit_bytes=56 * 1024 * 1024
        ),
        name=f"hidden_{layer}",
    )(normed, scale, coef, tg, tu, gate_weight, up_weight, down_weight)


def local(
    n,
    tokens,
    pre_gain,
    post_gain,
    gate_weight,
    up_weight,
    gate_taps,
    up_taps,
    gate_bias,
    up_bias,
    down_weight,
):
    width = tokens.shape[1] * n
    fl = gate_weight.shape[2]
    padding = -fl % LANES
    cut = fl // LANES * LANES
    pad_cols = lambda a: jnp.pad(a, ((0, 0),) * (a.ndim - 1) + ((0, padding),))
    if padding:
        tail = lambda a: jnp.pad(a[:, :, cut:], ((0, 0), (0, 0), (0, LANES - (fl - cut))))
        tails_gate, tails_up = tail(gate_weight), tail(up_weight)
    else:
        tails_gate = tails_up = jnp.zeros((gate_weight.shape[0], 16, LANES), jnp.bfloat16)
    coefs = pad_cols(
        jnp.concatenate(
            [gate_taps, gate_bias[:, None], up_taps, up_bias[:, None]], axis=1
        ).astype(jnp.float32)
    )
    state = tokens
    for layer in range(gate_weight.shape[0]):
        widened = state.astype(jnp.float32)
        pre_total = lax.psum(jnp.sum(widened * widened, axis=1), "ra")
        pre_scale = lax.rsqrt(pre_total / width + epsilon)[:, None]
        normed = (widened * pre_gain[layer].astype(jnp.float32)).astype(jnp.bfloat16)
        partial_value = down_partial(
            layer, n, normed, pre_scale, coefs[layer], tails_gate[layer], tails_up[layer],
            gate_weight, up_weight, down_weight,
        )
        branch = lax.psum(partial_value, "cb").astype(jnp.float32)
        post_total = lax.psum(jnp.sum(branch * branch, axis=1), "ra")
        post_scale = lax.rsqrt(post_total / width + epsilon)[:, None]
        state = (
            residual_scale * widened
            + branch * post_scale * post_gain[layer].astype(jnp.float32)
        ).astype(jnp.bfloat16)
    return state


def solution(mesh):
    in_specs = (
        P("grp", "ra"),
        P(None, "ra"),
        P(None, "ra"),
        P(None, "ra", "cb"),
        P(None, "ra", "cb"),
        P(None, None, "cb"),
        P(None, None, "cb"),
        P(None, "cb"),
        P(None, "cb"),
        P(None, "cb", "ra"),
    )
    body = functools.partial(local, mesh.shape["ra"])
    return jax.shard_map(
        body, mesh=mesh, in_specs=in_specs, out_specs=P("grp", "ra"), check_vma=False
    )
```

```python
import functools

import jax
import jax.numpy as jnp
from jax import lax
from jax.experimental import pallas as pl
from jax.experimental.pallas import tpu as pltpu
from jax.sharding import PartitionSpec as P

LEN = 256
LANES = 128
SKEW = 2

epsilon = 1e-06
residual_scale = 0.5
MESH = pl.DeviceIdType.MESH


def hidden_kernel(
    layer, n, nx, nch, nfull, fl,
    state_ref, pre_ref, post_ref, coef_ref, wg_hbm, wu_hbm, wd_hbm,
    out_ref,
    w, wd, part, hid, acc, normed, scale, branch, pair_out, pair_in, xbuf, fresh, pre_sq, post_sq,
    wsem, wtail, wdsem, part_send, part_recv, hid_send, hid_recv,
    pre_send, pre_recv, post_send, post_recv, x_send, x_recv, pair_send, pair_recv,
):
    z = lax.axis_index("ra")
    k = lax.axis_index("cb")
    core, xi = k % 2, k // 2
    peer = k + 1 - 2 * core
    tokens, dl = state_ref.shape
    half = tokens // 2
    width = dl * n
    tail = fl - nfull * LANES

    def w_copies(j):
        cols = pl.ds(pl.multiple_of(j * LANES, LANES), LANES)
        return (
            pltpu.make_async_copy(
                wg_hbm.at[layer, cols], w.at[j, pl.ds(0, LANES)], wsem.at[0, j]),
            pltpu.make_async_copy(
                wu_hbm.at[layer, cols], w.at[j, pl.ds(LANES, LANES)], wsem.at[1, j]),
        )

    def tail_copies():
        cols = pl.ds(nfull * LANES, tail)
        return (
            pltpu.make_async_copy(
                wg_hbm.at[layer, cols], w.at[nfull, pl.ds(0, tail)], wtail.at[0]),
            pltpu.make_async_copy(
                wu_hbm.at[layer, cols], w.at[nfull, pl.ds(LANES, tail)], wtail.at[1]),
        )

    barrier = pltpu.get_barrier_semaphore()

    @pl.loop(1, n)
    def _(o):
        pl.semaphore_signal(
            barrier, inc=1, device_id={"ra": (z + o) % n}, device_id_type=MESH)

    pl.semaphore_signal(barrier, inc=1, device_id={"cb": peer}, device_id_type=MESH)
    for o in range(1, nx):
        pl.semaphore_signal(
            barrier, inc=1, device_id={"cb": (xi + o) % nx * 2 + core}, device_id_type=MESH)

    @pl.loop(0, nfull)
    def _(j):
        for copy in w_copies(j):
            copy.start()

    if tail:
        for copy in tail_copies():
            copy.start()
    wd_copy = pltpu.make_async_copy(wd_hbm.at[layer], wd.at[pl.ds(0, fl)], wdsem)
    wd_copy.start()

    eye = lax.broadcasted_iota(jnp.int32, (LANES, LANES), 0) == lax.broadcasted_iota(
        jnp.int32, (LANES, LANES), 1)

    def to_row(column):
        return jnp.sum(jnp.where(eye, column, 0.0), axis=0, keepdims=True)

    def to_column(row):
        return jnp.sum(jnp.where(eye, row, 0.0), axis=1, keepdims=True)

    def sq_copy(buf, send, recv, o, slot):
        return pltpu.make_async_remote_copy(
            src_ref=buf.at[slot], dst_ref=buf.at[slot],
            send_sem=send.at[o], recv_sem=recv.at[slot],
            device_id={"ra": (z + o) % n}, device_id_type=MESH)

    def sq_start(buf, send, recv):
        @pl.loop(1, n)
        def _(o):
            sq_copy(buf, send, recv, o, z).start()

    def sq_wait(buf, send, recv):
        @pl.loop(1, n)
        def _(o):
            sq_copy(buf, send, recv, o, (z + o) % n).wait_recv()

    def scale_of(buf, group):
        total = buf[0, group : group + 1, :]
        for slot in range(1, n):
            total = total + buf[slot, group : group + 1, :]
        return to_column(lax.rsqrt(total / width + epsilon))

    pre_sq[z] = jnp.zeros(pre_sq.shape[1:], jnp.float32)
    post_sq[z] = jnp.zeros(post_sq.shape[1:], jnp.float32)
    for group in range(tokens // LANES):
        rows = slice(group * LANES, (group + 1) * LANES)
        wide = state_ref[rows, :].astype(jnp.float32)
        pre_sq[z, group : group + 1, :] = to_row(jnp.sum(wide * wide, axis=1, keepdims=True))
        normed[rows, :] = (wide * pre_ref[...]).astype(normed.dtype)

    if tail:
        for lo in (0, LANES):
            w[nfull, lo + tail : lo + LANES, :] = jnp.zeros((LANES - tail, dl), w.dtype)
        wd[fl:, :] = jnp.zeros((nch * LANES - fl, wd.shape[1]), wd.dtype)
    acc[...] = jnp.zeros_like(acc)

    pl.semaphore_wait(barrier, n - 1 + nx)
    sq_start(pre_sq, pre_send, pre_recv)

    def place(d):
        if d == 0:
            return n - 1 - z, z - 1, z + 1
        return z, z + 1, z - 1

    def part_copy(d, j, target):
        return pltpu.make_async_remote_copy(
            src_ref=part.at[d, j], dst_ref=part.at[d, j],
            send_sem=part_send.at[d, j], recv_sem=part_recv.at[d, j],
            device_id={"ra": target}, device_id_type=MESH)

    def hid_copy(d, j, target):
        return pltpu.make_async_remote_copy(
            src_ref=hid.at[d, j], dst_ref=hid.at[d, j],
            send_sem=hid_send.at[d, j], recv_sem=hid_recv.at[d, j],
            device_id={"ra": target}, device_id_type=MESH)

    def conv(values, taps, bias):
        rows = lax.broadcasted_iota(jnp.int32, values.shape, 0) % LEN
        count = len(taps)
        result = taps[count - 1] * values
        for offset in range(1, count):
            moved = jnp.where(rows >= offset, pltpu.roll(values, offset, 0), 0.0)
            result = result + taps[count - 1 - offset] * moved
        return result + bias

    def add_down(d, j):
        rows = slice(d * half, (d + 1) * half)
        wrows = pl.ds(pl.multiple_of(j * LANES, LANES), LANES)
        acc[rows, :] += jnp.dot(hid[d, j], wd[wrows, :], preferred_element_type=jnp.float32)

    @pl.loop(0, nch + 2 * (n - 1) * SKEW)
    def _(s):
        @pl.when(s < nfull)
        def _():
            for copy in w_copies(s):
                copy.wait()

        @pl.when(s == 1)
        def _():
            wd_copy.wait()
            if tail:
                for copy in tail_copies():
                    copy.wait()

        @pl.when(s == (n - 1) * SKEW)
        def _():
            sq_wait(pre_sq, pre_send, pre_recv)
            for group in range(tokens // LANES):
                scale[group * LANES : (group + 1) * LANES, :] = scale_of(pre_sq, group)

        for d in range(2):
            p, nxt, prv = place(d)
            rows = slice(d * half, (d + 1) * half)
            c = s - p * SKEW

            @pl.when((c >= 0) & (c < nch))
            def _():
                own = lax.dot_general(
                    normed[rows, :], w[c], (((1,), (1,)), ((), ())),
                    preferred_element_type=jnp.float32)

                @pl.when(p == 0)
                def _():
                    part[d, c] = own.astype(part.dtype)
                    part_copy(d, c, nxt).start()

                @pl.when((p > 0) & (p < n - 1))
                def _():
                    part_copy(d, c, nxt).wait_recv()
                    part[d, c] = (part[d, c].astype(jnp.float32) + own).astype(part.dtype)
                    part_copy(d, c, nxt).start()

                @pl.when(p == n - 1)
                def _():
                    part_copy(d, c, prv).wait_recv()
                    total = (part[d, c].astype(jnp.float32) + own) * scale[rows, :]
                    coef = coef_ref[:, pl.ds(pl.multiple_of(c * LANES, LANES), LANES)]
                    m = coef.shape[0] // 2
                    row = [coef[i : i + 1, :] for i in range(2 * m)]
                    gate = conv(total[:, :LANES], row[: m - 1], row[m - 1])
                    up = conv(total[:, LANES:], row[m : 2 * m - 1], row[2 * m - 1])
                    hid[d, c] = (jax.nn.gelu(gate, approximate=True) * up).astype(hid.dtype)
                    hid_copy(d, c, prv).start()
                    add_down(d, c)

            e = s - (2 * (n - 1) - p) * SKEW

            @pl.when((p < n - 1) & (e >= 0) & (e < nch))
            def _():
                hid_copy(d, e, nxt).wait_recv()

                @pl.when(p > 0)
                def _():
                    hid_copy(d, e, prv).start()

                add_down(d, e)

    kept = pl.ds(pl.multiple_of(core * half, half), half)
    given = pl.ds(pl.multiple_of((1 - core) * half, half), half)
    pair_copy = pltpu.make_async_remote_copy(
        src_ref=pair_out, dst_ref=pair_in,
        send_sem=pair_send.at[0], recv_sem=pair_recv.at[0],
        device_id={"cb": peer}, device_id_type=MESH)
    pair_out[...] = acc[given, :].astype(pair_out.dtype)
    pair_copy.start()
    pair_copy.wait_recv()
    xbuf[xi] = (acc[kept, :] + pair_in[...].astype(jnp.float32)).astype(xbuf.dtype)

    def x_copy(o, slot):
        return pltpu.make_async_remote_copy(
            src_ref=xbuf.at[slot], dst_ref=xbuf.at[slot],
            send_sem=x_send.at[o], recv_sem=x_recv.at[slot],
            device_id={"cb": (xi + o) % nx * 2 + core}, device_id_type=MESH)

    for o in range(1, nx):
        x_copy(o, xi).start()
    for o in range(1, nx):
        x_copy(o, (xi + o) % nx).wait_recv()
    for group in range(half // LANES):
        rows = slice(group * LANES, (group + 1) * LANES)
        total = xbuf[0, rows, :].astype(jnp.float32)
        for i in range(1, nx):
            total = total + xbuf[i, rows, :].astype(jnp.float32)
        branch[rows, :] = total
        post_sq[z, group : group + 1, :] = to_row(jnp.sum(total * total, axis=1, keepdims=True))
    sq_start(post_sq, post_send, post_recv)
    sq_wait(post_sq, post_send, post_recv)
    for group in range(half // LANES):
        rows = slice(group * LANES, (group + 1) * LANES)
        own = pl.ds(pl.multiple_of(core * half + group * LANES, LANES), LANES)
        fresh[own, :] = (
            residual_scale * state_ref[own, :].astype(jnp.float32)
            + branch[rows, :] * scale_of(post_sq, group) * post_ref[...]
        ).astype(fresh.dtype)

    state_copy = pltpu.make_async_remote_copy(
        src_ref=fresh.at[kept], dst_ref=fresh.at[kept],
        send_sem=pair_send.at[1], recv_sem=pair_recv.at[1],
        device_id={"cb": peer}, device_id_type=MESH)
    state_copy.start()
    out_ref[kept, :] = fresh[kept, :]
    pltpu.make_async_remote_copy(
        src_ref=fresh.at[given], dst_ref=fresh.at[given],
        send_sem=pair_send.at[1], recv_sem=pair_recv.at[1],
        device_id={"cb": peer}, device_id_type=MESH).wait_recv()
    out_ref[given, :] = fresh[given, :]

    pair_copy.wait_send()
    state_copy.wait_send()
    for o in range(1, nx):
        x_copy(o, xi).wait_send()

    @pl.loop(1, n)
    def _(o):
        sq_copy(pre_sq, pre_send, pre_recv, o, z).wait_send()
        sq_copy(post_sq, post_send, post_recv, o, z).wait_send()

    for d in range(2):
        p, nxt, prv = place(d)

        @pl.loop(0, nch)
        def _(j):
            @pl.when(p < n - 1)
            def _():
                part_copy(d, j, nxt).wait_send()

            @pl.when(p > 0)
            def _():
                hid_copy(d, j, prv).wait_send()


def sublayer(layer, n, nx, state, pre, post, coef, gate_weight, up_weight, down_weight):
    tokens, dl = state.shape
    fl = gate_weight.shape[1]
    nfull = fl // LANES
    nch = -(-fl // LANES)
    half = tokens // 2
    sq_rows = -(-(tokens // LANES) // 8) * 8
    vmem = pl.BlockSpec(memory_space=pltpu.VMEM)
    hbm = pl.BlockSpec(memory_space=pl.ANY)
    dma = pltpu.SemaphoreType.DMA
    bf16, f32 = jnp.bfloat16, jnp.float32
    return pl.pallas_call(
        functools.partial(hidden_kernel, layer, n, nx, nch, nfull, fl),
        out_shape=jax.ShapeDtypeStruct((tokens, dl), bf16),
        in_specs=[vmem] * 4 + [hbm] * 3,
        out_specs=vmem,
        scratch_shapes=[
            pltpu.VMEM((nch, 2 * LANES, dl), bf16),
            pltpu.VMEM((nch * LANES, dl), bf16),
            pltpu.VMEM((2, nch, half, 2 * LANES), bf16),
            pltpu.VMEM((2, nch, half, LANES), bf16),
            pltpu.VMEM((tokens, dl), f32),
            pltpu.VMEM((tokens, dl), bf16),
            pltpu.VMEM((tokens, 1), f32),
            pltpu.VMEM((half, dl), f32),
            pltpu.VMEM((half, dl), bf16),
            pltpu.VMEM((half, dl), bf16),
            pltpu.VMEM((nx, half, dl), bf16),
            pltpu.VMEM((tokens, dl), bf16),
            pltpu.VMEM((n, sq_rows, LANES), f32),
            pltpu.VMEM((n, sq_rows, LANES), f32),
            dma((2, nch)),
            dma((2,)),
            dma,
            dma((2, nch)),
            dma((2, nch)),
            dma((2, nch)),
            dma((2, nch)),
            dma((n,)),
            dma((n,)),
            dma((n,)),
            dma((n,)),
            dma((nx,)),
            dma((nx,)),
            dma((2,)),
            dma((2,)),
        ],
        compiler_params=pltpu.CompilerParams(
            collective_id=layer, has_side_effects=True, vmem_limit_bytes=56 * 1024 * 1024
        ),
        name=f"hidden_{layer}",
    )(state, pre, post, coef, gate_weight, up_weight, down_weight)


def local(
    n,
    nx,
    tokens,
    pre_gain,
    post_gain,
    gate_weight,
    up_weight,
    gate_taps,
    up_taps,
    gate_bias,
    up_bias,
    down_weight,
):
    padding = -gate_weight.shape[2] % LANES
    coefs = jnp.concatenate(
        [gate_taps, gate_bias[:, None], up_taps, up_bias[:, None]], axis=1
    ).astype(jnp.float32)
    coefs = jnp.pad(coefs, ((0, 0), (0, 0), (0, padding)))
    pre, post = pre_gain.astype(jnp.float32), post_gain.astype(jnp.float32)
    gate_cols = jnp.swapaxes(gate_weight, 1, 2)
    up_cols = jnp.swapaxes(up_weight, 1, 2)
    state = tokens
    for layer in range(gate_weight.shape[0]):
        state = sublayer(
            layer, n, nx, state, pre[layer : layer + 1], post[layer : layer + 1], coefs[layer],
            gate_cols, up_cols, down_weight,
        )
    return state


def solution(mesh):
    in_specs = (
        P("grp", "ra"),
        P(None, "ra"),
        P(None, "ra"),
        P(None, "ra", "cb"),
        P(None, "ra", "cb"),
        P(None, None, "cb"),
        P(None, None, "cb"),
        P(None, "cb"),
        P(None, "cb"),
        P(None, "cb", "ra"),
    )
    body = functools.partial(local, mesh.shape["ra"], mesh.shape["cb"] // 2)
    return jax.shard_map(
        body, mesh=mesh, in_specs=in_specs, out_specs=P("grp", "ra"), check_vma=False
    )
```
